1024 devices in a mesh: fs: 256 (over z, x, core), tp: 4 (over y).
Axes of the slice: x: 4, y: 4, z: 32, core: 2. Of those that a mesh axis runs over, the one named last changes fastest.
Arguments:
- saved_inputs: bfloat16 [131072, 2048], P('fs'), may hold values from -6 to 6
- unit_cotangent: bfloat16 [131072, 2560], P('fs', 'tp'), may hold values from -0.049560547 to 0.049560547
- gated_states: bfloat16 [131072, 2560], P('fs', 'tp'), may hold values from -6 to 6
- mixer_cotangent: bfloat16 [131072, 2048], P('fs'), may hold values from -0.049560547 to 0.049560547
- left_factor: bfloat16 [2048, 256], replicated, may hold values from -0.125 to 0.125
- right_factor: bfloat16 [2048, 256], replicated, may hold values from -0.125 to 0.125
- master_input: float32 [2048, 2560], P('fs', 'tp'), may hold values from -6 to 6
- master_output: float32 [2560, 2048], P('tp', 'fs'), may hold values from -6 to 6
- moment_input: float32 [256, 2560], P('fs', 'tp'), may hold values from -80 to 80
- moment_output: float32 [256, 2560], P('fs', 'tp'), may hold values from -80 to 80
- square_input: float32 [256, 2560], P('fs', 'tp'), may hold values from 0.1 to 4
- square_output: float32 [256, 2560], P('fs', 'tp'), may hold values from 0.1 to 4
Outputs:
- first_input: float32 [256, 2560], P('fs', 'tp')
- first_output: float32 [256, 2560], P('fs', 'tp')
- second_input: float32 [256, 2560], P('fs', 'tp')
- second_output: float32 [256, 2560], P('fs', 'tp')
- step_input: float32 [2048, 2560], P('fs', 'tp')
- step_output: float32 [2560, 2048], P('tp', 'fs')
- weight_input: float32 [2048, 2560], P('fs', 'tp')
- weight_output: float32 [2560, 2048], P('tp', 'fs')
- copy_input: bfloat16 [2048, 2560], P('fs', 'tp')
- copy_output: bfloat16 [2560, 2048], P('tp', 'fs')
The draws below stay inside these ranges and needn't reach their ends.
All inputs are finite; a program needn't handle non-finite values.
Results may differ from the reference program's by a relative error of at most 0.002.
Values sent between devices are 32-bit elements; how exact they have to be, the bound alone decides.
A program may use at most 32 MiB of HBM per device.

```python
import math
import jax
import jax.numpy as jnp
from jax import lax

D = 2048
R = 2560
RANK = 256
TOKENS = 131072


def moment_field(key):
    rows = jnp.arange(RANK, dtype=jnp.float32) / (RANK - 1)
    cols = jnp.arange(R, dtype=jnp.float32) / (R - 1)
    scale = 0.05 * (10.0 ** rows)[:, None] * (10.0 ** cols)[None, :]
    rough = jnp.exp(jax.random.uniform(jax.random.fold_in(key, 11), (RANK, R), jnp.float32, -0.69, 0.69))
    values = jax.random.truncated_normal(jax.random.fold_in(key, 13), -4.0, 4.0, (RANK, R), jnp.float32)
    return 2.0 * scale * rough * values


def draw_moment_input(key, part):
    return moment_field(jax.random.fold_in(key, 1))


def draw_moment_output(key, part):
    return moment_field(jax.random.fold_in(key, 2))


def levels(rng, shape, cuts, least, high):
    level = 1.0
    for position, shards_of in cuts:
        draws = jax.random.uniform(jax.random.fold_in(jax.random.fold_in(rng, 6), position), (shards_of,), jnp.float32, least / len(cuts), high / len(cuts))
        level = level * jnp.repeat(jnp.exp(draws), shape[position] // shards_of).reshape((-1,) + (1,) * (len(shape) - 1 - position))
    return level


def bell_draw(key, dims, spread, reach, split=(), kind=jnp.bfloat16):
    factor_of = levels(key, dims, split, -0.22, 0.18) if split else 1.0
    array = jax.random.normal(key, dims, jnp.float32) * spread * factor_of
    return jnp.minimum(jnp.maximum(array, -reach), reach).astype(kind)


def setup_inputs(seed: int = 0) -> dict:
    key_list = jax.random.split(jax.random.key(seed), 13)
    return {
        "saved_inputs": bell_draw(key_list[0], (TOKENS, D), 1.0, 6.0, ((0, 256),)),
        "unit_cotangent": bell_draw(key_list[1], (TOKENS, R), (3.0 / TOKENS ** 0.5), 0.049560547, ((0, 256), (1, 4))),
        "gated_states": bell_draw(key_list[2], (TOKENS, R), 1.0, 6.0, ((0, 256), (1, 4))),
        "mixer_cotangent": bell_draw(key_list[3], (TOKENS, D), (3.0 / TOKENS ** 0.5), 0.049560547, ((0, 256),)),
        "left_factor": bell_draw(key_list[4], (D, RANK), D ** -0.5, 0.125),
        "right_factor": bell_draw(key_list[5], (D, RANK), D ** -0.5, 0.125),
        "master_input": bell_draw(key_list[6], (D, R), 1.0, 6.0, ((0, 256), (1, 4)), jnp.float32),
        "master_output": bell_draw(key_list[7], (R, D), 1.0, 6.0, ((0, 4), (1, 256)), jnp.float32),
        "moment_input": draw_moment_input(jax.random.fold_in(key_list[12], 71), 0),
        "moment_output": draw_moment_output(jax.random.fold_in(key_list[12], 71), 0),
        "square_input": jnp.clip(jnp.exp(math.log(4.0) - 3.6888794 * jax.random.uniform(key_list[10], (RANK, R), jnp.float32) ** levels(key_list[10], (RANK, R), ((0, 256), (1, 4)), -0.2, 0.2)), 0.1, 4.0),
        "square_output": jnp.clip(jnp.exp(math.log(4.0) - 3.6888794 * jax.random.uniform(key_list[11], (RANK, R), jnp.float32) ** levels(key_list[11], (RANK, R), ((0, 256), (1, 4)), -0.2, 0.2)), 0.1, 4.0),
    }


def contract_tokens(left, right):
    return lax.dot_general(left, right, (((0,), (0,)), ((), ())), preferred_element_type=jnp.float32)

def moment_update(moment, square, projected):
    first = 0.9 * moment + 0.1 * projected
    second = 0.95 * square + 0.05 * projected * projected
    heading = first / (jnp.sqrt(second) + 1e-08)
    gain = jnp.minimum(1.0, 0.1 / jnp.sqrt(jnp.mean(heading * heading) + 1e-06))
    return (first, second, heading, gain)

def reference(saved_inputs, unit_cotangent, gated_states, mixer_cotangent, left_factor, right_factor, master_input, master_output, moment_input, moment_output, square_input, square_output):
    in_rows = jnp.dot(saved_inputs, left_factor, preferred_element_type=jnp.float32).astype(jnp.bfloat16)
    out_rows = jnp.dot(mixer_cotangent, right_factor, preferred_element_type=jnp.float32).astype(jnp.bfloat16)
    in_proj = contract_tokens(in_rows, unit_cotangent)
    out_proj = contract_tokens(out_rows, gated_states)
    first_input, second_input, heading_input, gain_input = moment_update(moment_input, square_input, in_proj)
    first_output, second_output, heading_output, gain_output = moment_update(moment_output, square_output, out_proj)
    step_input = gain_input * jnp.dot(left_factor.astype(jnp.float32), heading_input, precision=lax.Precision.HIGHEST)
    step_output = gain_output * jnp.dot(right_factor.astype(jnp.float32), heading_output, precision=lax.Precision.HIGHEST).T
    weight_input = master_input - step_input
    weight_output = master_output - step_output
    return (first_input, first_output, second_input, second_output, step_input, step_output, weight_input, weight_output, weight_input.astype(jnp.bfloat16), weight_output.astype(jnp.bfloat16))
```

```python
import functools

import jax
import jax.numpy as jnp
from jax import lax
from jax.experimental import pallas as pl
from jax.experimental.pallas import tpu as pltpu
from jax.sharding import Mesh
from jax.sharding import PartitionSpec as P

FS = ("fs_0", "fs_1", "fs_2")
MESH = pl.DeviceIdType.MESH

first_decay = 0.9
second_decay = 0.95
divide_guard = 1e-08
mean_guard = 1e-06
clip_level = 0.1


def near(x):
    return x + 1 - 2 * lax.rem(x, 2)


def permutation(nz, nx):
    n = 2 * nz * nx
    p = lax.broadcasted_iota(jnp.int32, (n, n), 0)
    r = lax.broadcasted_iota(jnp.int32, (n, n), 1)
    bits_z = (2 * nz).bit_length() - 1
    bits_x = (2 * nx).bit_length() - 1
    px = lax.shift_right_logical(p, bits_z)
    rest = lax.bitwise_and(p, 2 * nz - 1)
    pz = lax.shift_right_logical(rest, 1)
    pc = lax.bitwise_and(rest, 1)
    want = lax.shift_left(pz, bits_x) + 2 * px + pc
    return jnp.where(want == r, 1.0, 0.0).astype(jnp.bfloat16)


def dot_t(a, b):
    return lax.dot_general(a, b, (((1,), (1,)), ((), ())), preferred_element_type=jnp.float32)


def exchange(
    nz, nx, ny, entries,
    a0, u0, u1, a1, l0, l1, m0, m1, s0, s1,
    out_step, out_fs,
    X, F, U, PS, CR, S, XA, XB, FA, FB, XA2, XB2, T, ZS, ZR, ZG, HX, MS, MR, FO, Q, QY, QX, ST,
    load_sem, core_send, core_recv, x_send, x_recv, z_send, z_recv, q_send, q_recv,
):
    z = lax.axis_index("fs_0")
    x = lax.axis_index("fs_1")
    c = lax.axis_index("fs_2")
    y = lax.axis_index("tp")
    other = 1 - c
    xa = near(x)
    xb = nx - 1 - x
    xo = lax.rem(x + 2, nx)
    nh = nz
    W = u0.shape[1]

    def z_offset(i):
        step = lax.div(i, 2)
        return lax.rem(z + nz + (nz // 2 - step) * (1 - 2 * lax.rem(i, 2)) + nz, nz)

    barrier = pltpu.get_barrier_semaphore()

    def greet(i, carry):
        pl.semaphore_signal(barrier, inc=1, device_id={"fs_0": z_offset(i)}, device_id_type=MESH)
        return carry

    lax.fori_loop(0, nz - 1, lambda i, t: greet(jnp.where(i == 0, 0, i + 1), t), 0)
    pl.semaphore_signal(barrier, inc=1, device_id={"fs_2": other}, device_id_type=MESH)
    for d in range(1, nx):
        pl.semaphore_signal(barrier, inc=1, device_id={"fs_1": lax.rem(x + d, nx)}, device_id_type=MESH)
    for d in range(1, ny):
        pl.semaphore_signal(barrier, inc=1, device_id={"tp": lax.rem(y + d, ny)}, device_id_type=MESH)

    loads = []
    for k, (src, dst) in enumerate((
        (l0, F.at[0]), (a0, X.at[0]), (u0, U.at[0]),
        (l1, F.at[1]), (a1, X.at[1]), (u1, U.at[1]),
        (m0, MS.at[0, 0]), (s0, MS.at[0, 1]), (m1, MS.at[1, 0]), (s1, MS.at[1, 1]),
    )):
        cp = pltpu.make_async_copy(src, dst, load_sem.at[k])
        cp.start()
        loads.append(cp)
    perm = permutation(nz, nx)
    for cp in loads:
        cp.wait()

    def project(k, carry):
        m = lax.rem(other + k, 2)
        rows = jnp.dot(X[m], F[m], preferred_element_type=jnp.float32).astype(jnp.bfloat16)
        turned = dot_t(perm, rows).astype(jnp.bfloat16)
        PS[m] = jnp.dot(turned, U[m], preferred_element_type=jnp.float32)
        return carry

    lax.fori_loop(0, 2, project, 0)

    pl.semaphore_wait(barrier, 1 + (nx - 1) + (ny - 1) + (nz - 1))

    def remote(src, dst, send, recv, **where):
        return pltpu.make_async_remote_copy(
            src_ref=src, dst_ref=dst, send_sem=send, recv_sem=recv, device_id=where, device_id_type=MESH
        )

    give = remote(PS.at[other], CR, core_send.at[0], core_recv.at[0], fs_2=other)
    give.start()
    give_m = remote(MS.at[other], MR, core_send.at[1], core_recv.at[1], fs_2=other)
    give_m.start()
    give.wait_recv()
    S[...] = (PS[c] + CR[...]).reshape(nx, 2 * nz, W)

    lo, hi = pl.ds(0, nh), pl.ds(nh, nh)
    c_a1 = remote(S.at[xo, lo], XA.at[1], x_send.at[0], x_recv.at[0], fs_1=xa)
    c_b1 = remote(S.at[xo, hi], XB.at[1], x_send.at[1], x_recv.at[1], fs_1=xb)
    c_a0 = remote(S.at[xa, lo], XA.at[0], x_send.at[2], x_recv.at[2], fs_1=xa)
    c_b0 = remote(S.at[xb, hi], XB.at[0], x_send.at[3], x_recv.at[3], fs_1=xb)
    for cp in (c_a1, c_b1, c_a0, c_b0):
        cp.start()
    c_a1.wait_recv()
    FA[...] = S[xb, 0:nh] + XA[1]
    c_fa = remote(FA, XA2, x_send.at[4], x_recv.at[4], fs_1=xb)
    c_fa.start()
    c_b1.wait_recv()
    FB[...] = S[xa, nh : 2 * nh] + XB[1]
    c_fb = remote(FB, XB2, x_send.at[5], x_recv.at[5], fs_1=xa)
    c_fb.start()
    c_a0.wait_recv()
    T[0:nh] = S[x, 0:nh] + XA[0]
    c_b0.wait_recv()
    T[nh : 2 * nh] = S[x, nh : 2 * nh] + XB[0]
    c_fa.wait_recv()
    T[0:nh] = T[0:nh] + XA2[...]
    c_fb.wait_recv()
    T[nh : 2 * nh] = T[nh : 2 * nh] + XB2[...]
    for j in range(nz):
        ZS[j] = T[2 * j : 2 * j + 2]

    def scatter(i, carry):
        t = z_offset(jnp.where(i == 0, 0, i + 1))
        remote(ZS.at[t], ZR.at[i], z_send.at[0], z_recv.at[0], fs_0=t).start()
        return carry

    lax.fori_loop(0, nz - 1, scatter, 0)
    all_in = remote(ZR, ZR, z_send.at[0], z_recv.at[0], fs_0=lax.rem(z + 1, nz))
    all_in.wait_recv()
    proj = ZS[z] + jnp.sum(ZR[...], axis=0)

    give_m.wait_recv()

    def both(own, got):
        top = jnp.where(c == 0, own, got)
        low = jnp.where(c == 0, got, own)
        return jnp.concatenate([top, low], axis=0)

    moment = both(MS[c, 0], MR[0])
    square = both(MS[c, 1], MR[1])
    first = first_decay * moment + (1.0 - first_decay) * proj
    second = second_decay * square + (1.0 - second_decay) * proj * proj
    heading = first / (jnp.sqrt(second) + divide_guard)
    ZG[z] = heading

    def spread(i, carry):
        t = z_offset(jnp.where(i == 0, 0, i + 1))
        remote(ZG.at[z], ZG.at[z], z_send.at[1], z_recv.at[1], fs_0=t).start()
        return carry

    lax.fori_loop(0, nz - 1, spread, 0)

    out_fs[c, 0] = jnp.where(c == 0, first[0:1], first[1:2])
    out_fs[c, 1] = jnp.where(c == 0, second[0:1], second[1:2])
    FO[0] = jnp.where(c == 0, first[1:2], first[0:1])
    FO[1] = jnp.where(c == 0, second[1:2], second[0:1])
    give_f = remote(FO, out_fs.at[c], core_send.at[2], core_recv.at[2], fs_2=other)
    give_f.start()

    start = pl.multiple_of((z * nx + x) * 16, 16)
    factor = dot_t(F[c, pl.ds(start, 16), :], perm)

    all_out = remote(ZR, ZR, z_send.at[1], z_recv.at[1], fs_0=lax.rem(z + 1, nz))
    all_out.wait_recv()
    for j in range(nz):
        HX[x, 2 * j : 2 * j + 2] = ZG[j]

    g = [
        remote(HX.at[x, lo], HX.at[x, lo], x_send.at[6], x_recv.at[6], fs_1=xb),
        remote(HX.at[x, hi], HX.at[x, hi], x_send.at[7], x_recv.at[7], fs_1=xa),
        remote(HX.at[x, lo], HX.at[x, lo], x_send.at[8], x_recv.at[8], fs_1=xa),
        remote(HX.at[x, hi], HX.at[x, hi], x_send.at[9], x_recv.at[9], fs_1=xb),
    ]
    for cp in g:
        cp.start()

    mine = HX[x]
    squares = jnp.sum((mine * mine).reshape(2 * nz // 8, 8, W), axis=0)
    total = squares[:, 0:128]
    for k in range(1, W // 128):
        total = total + squares[:, k * 128 : (k + 1) * 128]
    Q[0] = total
    if ny > 1:
        for d in range(1, ny):
            remote(Q.at[0], QY.at[d - 1], q_send.at[0], q_recv.at[0], tp=lax.rem(y + d, ny)).start()

    g[0].wait_recv()
    f0 = remote(HX.at[xb, lo], HX.at[xb, lo], x_send.at[10], x_recv.at[10], fs_1=xa)
    f0.start()
    g[1].wait_recv()
    f1 = remote(HX.at[xa, hi], HX.at[xa, hi], x_send.at[11], x_recv.at[11], fs_1=xb)
    f1.start()

    if ny > 1:
        y_all = remote(QY, QY, q_send.at[0], q_recv.at[0], tp=lax.rem(y + 1, ny))
        y_all.wait_recv()
        total = total + jnp.sum(QY[...], axis=0)
    Q[1] = total
    for d in range(1, nx):
        remote(Q.at[1], QX.at[d - 1], q_send.at[1], q_recv.at[1], fs_1=lax.rem(x + d, nx)).start()
    x_all = remote(QX, QX, q_send.at[1], q_recv.at[1], fs_1=lax.rem(x + 1, nx))
    x_all.wait_recv()
    total = total + jnp.sum(QX[...], axis=0)
    mean = jnp.sum(jnp.sum(total, axis=1, keepdims=True), axis=0, keepdims=True) / entries
    gain = jnp.minimum(1.0, clip_level / jnp.sqrt(mean + mean_guard))

    for cp in (g[2], g[3], f0, f1):
        cp.wait_recv()
    block = jnp.dot(
        factor, HX[...].reshape(2 * nz * nx, W),
        precision=lax.Precision.HIGHEST, preferred_element_type=jnp.float32,
    )
    step = gain * block
    ST[...] = step.reshape(2, 8, W)
    give_s = remote(ST.at[other], out_step.at[c], core_send.at[3], core_recv.at[3], fs_2=other)
    give_s.start()
    out_step[c] = ST[c]

    give.wait_send()
    give_m.wait_send()
    for cp in (c_a1, c_b1, c_a0, c_b0, c_fa, c_fb, *g, f0, f1):
        cp.wait_send()
    all_in.wait_send()
    all_out.wait_send()
    if ny > 1:
        y_all.wait_send()
    x_all.wait_send()
    give_f.wait()
    give_s.wait()


def finish(step, fs, mi, mo, fi, fo, si, so, ti, to, wi, wo, ci, co):
    fi[...] = fs[0, 0]
    si[...] = fs[0, 1]
    fo[...] = fs[1, 0]
    so[...] = fs[1, 1]
    s = step[0]
    ti[...] = s
    w = mi[...] - s
    wi[...] = w
    ci[...] = w.astype(jnp.bfloat16)
    s = step[1]
    to[...] = s
    w = mo[...] - s
    wo[...] = w
    co[...] = w.astype(jnp.bfloat16)


def shards(nz, nx, ny, saved, unit, gated, mixer, left, right, mi, mo, m0, m1, s0, s1):
    f32, bf16 = jnp.float32, jnp.bfloat16
    n, d = saved.shape
    W = unit.shape[1]
    rank = left.shape[1]
    assert rank == 2 * nz * nx and nx == 4 and mi.shape[0] == 8 and m0.shape[0] == 1
    entries = float(rank * W * ny)
    V = pltpu.VMEM
    dma = pltpu.SemaphoreType.DMA
    half = nz
    anywhere = pl.BlockSpec(memory_space=pl.ANY)
    vmem = pl.BlockSpec(memory_space=pltpu.VMEM)
    step, fs = pl.pallas_call(
        functools.partial(exchange, nz, nx, ny, entries),
        out_shape=(
            jax.ShapeDtypeStruct((2, 8, W), f32),
            jax.ShapeDtypeStruct((2, 2, 1, W), f32),
        ),
        in_specs=[anywhere] * 10,
        out_specs=(vmem, vmem),
        scratch_shapes=[
            V((2, n, d), bf16),
            V((2, d, rank), bf16),
            V((2, n, W), bf16),
            V((2, rank, W), f32),
            V((rank, W), f32),
            V((nx, 2 * nz, W), f32),
            V((2, half, W), f32),
            V((2, half, W), f32),
            V((half, W), f32),
            V((half, W), f32),
            V((half, W), f32),
            V((half, W), f32),
            V((2 * nz, W), f32),
            V((nz, 2, W), f32),
            V((nz - 1, 2, W), f32),
            V((nz, 2, W), f32),
            V((nx, 2 * nz, W), f32),
            V((2, 2, 1, W), f32),
            V((2, 1, W), f32),
            V((2, 1, W), f32),
            V((2, 8, 128), f32),
            V((max(ny - 1, 1), 8, 128), f32),
            V((nx - 1, 8, 128), f32),
            V((2, 8, W), f32),
            dma((10,)),
            dma((4,)),
            dma((4,)),
            dma((12,)),
            dma((12,)),
            dma((2,)),
            dma((2,)),
            dma((2,)),
            dma((2,)),
        ],
        compiler_params=pltpu.CompilerParams(collective_id=0, has_side_effects=True),
        name="exchange",
    )(saved, unit, gated, mixer, left, right, m0, m1, s0, s1)
    row = jax.ShapeDtypeStruct((1, W), f32)
    outs = pl.pallas_call(
        finish,
        out_shape=(
            row, row, row, row,
            jax.ShapeDtypeStruct((8, W), f32),
            jax.ShapeDtypeStruct((8, W), f32),
            jax.ShapeDtypeStruct((8, W), f32),
            jax.ShapeDtypeStruct((8, W), f32),
            jax.ShapeDtypeStruct((8, W), bf16),
            jax.ShapeDtypeStruct((8, W), bf16),
        ),
        name="finish",
    )(step, fs, mi, mo.T)
    return tuple(out.T if k in (5, 7, 9) else out for k, out in enumerate(outs))


def solution(mesh):
    ny = mesh.shape["tp"]
    nx = 4
    nz = mesh.shape["fs"] // (2 * nx)
    finer = Mesh(mesh.devices.reshape(nz, nx, 2, ny), (*FS, "tp"))
    rows, cols = P(FS, "tp"), P("tp", FS)
    return jax.shard_map(
        functools.partial(shards, nz, nx, ny),
        mesh=finer,
        in_specs=(P(FS, None), rows, rows, P(FS, None), P(), P(), rows, cols, rows, rows, rows, rows),
        out_specs=(rows, rows, rows, rows, rows, cols, rows, cols, rows, cols),
        check_vma=False,
    )
```

```python
import functools

import jax
import jax.numpy as jnp
from jax import lax
from jax.experimental import pallas as pl
from jax.experimental.pallas import tpu as pltpu
from jax.sharding import Mesh
from jax.sharding import PartitionSpec as P

FS = ("fs_0", "fs_1", "fs_2")
MESH = pl.DeviceIdType.MESH

first_decay = 0.9
second_decay = 0.95
divide_guard = 1e-08
mean_guard = 1e-06
clip_level = 0.1


def groups_of(nz):
    return min(4, nz // 2)


def permutation(nz, nx, base):
    n = 2 * nz * nx
    pairs = nz // 2
    E = pairs // groups_of(nz)
    p = lax.broadcasted_iota(jnp.int32, (n, n), 0)
    r = lax.broadcasted_iota(jnp.int32, (n, n), 1)
    log = lambda v: v.bit_length() - 1
    shift, mask = lax.shift_right_logical, lax.bitwise_and
    k = shift(p, log(4 * E * nx)) * E + mask(shift(p, 1), E - 1)
    parity = mask(shift(p, log(2 * E)), 1)
    px = mask(shift(p, log(4 * E)), nx - 1)
    reach = pairs // 2 - shift(k + 1, 1)
    offset = jnp.where(mask(k, 1) == 1, reach, -reach)
    target = mask(base + nz + 2 * offset + parity, nz - 1)
    want = target * (2 * nx) + 2 * px + mask(p, 1)
    return jnp.where(want == r, 1.0, 0.0).astype(jnp.bfloat16)


def dot_t(a, b):
    return lax.dot_general(a, b, (((1,), (1,)), ((), ())), preferred_element_type=jnp.float32)


def exchange(
    nz, nx, ny,
    a0, u0, u1, a1, l0, l1, m0, m1, s0, s1,
    out_step, out_fs, out_q,
    X, F, U, PS, CR, S, XR, TP, PR, ZS, ZR, ZG, HX, MS, MR, FO, QY, QZ, QP, ST,
    load_sem, small_sem, core_send, core_recv, x_send, x_recv, p_send, p_recv,
    z_send, z_recv, g_recv, h_send, h_recv, q_send, q_recv, ready,
):
    z = lax.axis_index("fs_0")
    x = lax.axis_index("fs_1")
    c = lax.axis_index("fs_2")
    y = lax.axis_index("tp")
    other = 1 - c
    W = u0.shape[1]
    tokens = a0.shape[0] // 2
    NG = groups_of(nz)
    NP = nz // 2
    E = NP // NG
    HR = 2 * E
    GR = 2 * HR
    b = lax.rem(z, 2)
    base = z - b
    twin = base + 1 - b
    reach = max(2, nz // 8)

    def z_at(offset):
        return lax.rem(z + nz + offset, nz)

    def z_target(k):
        far = NP // 2 - lax.div(k + 1, 2)
        return z_at(2 * far * (2 * lax.rem(k, 2) - 1))

    def around(j):
        return {
            "fs_0": base + lax.rem(b + lax.rem(lax.div(j, nx), 2), 2),
            "fs_1": lax.rem(x + lax.rem(j, nx), nx),
            "fs_2": lax.rem(c + lax.div(j, 2 * nx), 2),
        }

    with jax.named_scope("p00_loads"):
        sources = ((l0, a0, u0), (l1, a1, u1))
        halves = (pl.ds(0, tokens), pl.ds(tokens, tokens))

        def parts(m):
            l, a, u = sources[m]
            return (
                (l, F.at[m]), (a.at[halves[0]], X.at[m, 0]), (a.at[halves[1]], X.at[m, 1]), (u, U.at[m]),
            )

        for mine in range(2):

            @pl.when(c == mine)
            def _(mine=mine):
                for m in (1 - mine, mine):
                    for k, (src, dst) in enumerate(parts(m)):
                        pltpu.make_async_copy(src, dst, load_sem.at[m, k]).start()

        small = []
        for k, (src, dst) in enumerate((
            (m0, MS.at[0, 0]), (s0, MS.at[0, 1]), (m1, MS.at[1, 0]), (s1, MS.at[1, 1]),
        )):
            cp = pltpu.make_async_copy(src, dst, small_sem.at[k])
            cp.start()
            small.append(cp)

    with jax.named_scope("p01_greet"):
        barrier = pltpu.get_barrier_semaphore()
        met = 0
        for d in range(reach, 0, -2):
            for offset in (d, -d):
                pl.semaphore_signal(barrier, inc=1, device_id={"fs_0": z_at(offset)}, device_id_type=MESH)
                met += 1
        for d in range(1, ny):
            pl.semaphore_signal(barrier, inc=1, device_id={"tp": lax.rem(y + d, ny)}, device_id_type=MESH)
            met += 1

        def greet(j, carry):
            pl.semaphore_signal(barrier, inc=1, device_id=around(j), device_id_type=MESH)
            return carry

        lax.fori_loop(1, 4 * nx, greet, 0)
        met += 4 * nx - 1

    perm = permutation(nz, nx, base)

    def arrived(m, k):
        src, dst = parts(0)[k]
        dst = (F.at[m], X.at[m, 0], X.at[m, 1], U.at[m])[k]
        pltpu.make_async_copy(src, dst, load_sem.at[m, k]).wait()

    def project(m):
        arrived(m, 0)
        turned = []
        for h in range(2):
            arrived(m, 1 + h)
            rows = jnp.dot(X[m, h], F[m], preferred_element_type=jnp.float32).astype(jnp.bfloat16)
            turned.append(dot_t(perm, rows).astype(jnp.bfloat16))
        arrived(m, 3)
        sums = jnp.dot(jnp.concatenate(turned, axis=1), U[m], preferred_element_type=jnp.float32)
        PS[m] = sums.reshape(NG, nx * GR, W)

    def remote(src, dst, send, recv, **where):
        return pltpu.make_async_remote_copy(
            src_ref=src, dst_ref=dst, send_sem=send, recv_sem=recv, device_id=where, device_id_type=MESH
        )

    with jax.named_scope("p02_project"):
        project(other)
        for cp in small:
            cp.wait()
    with jax.named_scope("p03_barrier"):
        pl.semaphore_wait(barrier, met)

    for offset in (reach, -reach):
        pl.semaphore_signal(ready.at[0], inc=1, device_id={"fs_0": z_at(offset)}, device_id_type=MESH)

    give = [
        remote(PS.at[other, g], CR.at[g], core_send.at[g], core_recv.at[g], fs_2=other) for g in range(NG)
    ]
    for cp in give:
        cp.start()
    give_m = remote(MS.at[other], MR, core_send.at[NG], core_recv.at[NG], fs_2=other)
    give_m.start()
    with jax.named_scope("p04_project"):
        project(c)

    x_order = (2, 1, 3)
    with jax.named_scope("p05_xsend"):
        for g in range(NG):
            give[g].wait_recv()
            S[g] = (PS[c, g] + CR[g]).reshape(nx, GR, W)
            for d in x_order:
                t = lax.rem(x + d, nx)
                remote(S.at[g, t], XR.at[g, d - 1], x_send.at[0], x_recv.at[g], fs_1=t).start()

    with jax.named_scope("p06_ready"):
        pl.semaphore_wait(ready.at[0], 2)
        for offset in (2 * reach, -2 * reach):
            pl.semaphore_signal(ready.at[1], inc=1, device_id={"fs_0": z_at(offset)}, device_id_type=MESH)

    next_x = lax.rem(x + 1, nx)
    next_z = z_at(2)

    def sum_x(g):
        with jax.named_scope(f"p07_x{g}"):
            remote(XR.at[g], XR.at[g], x_send.at[0], x_recv.at[g], fs_1=next_x).wait_recv()
            part = S[g, x] + (XR[g, 0] + XR[g, 1] + XR[g, 2])
            TP[g] = part.reshape(2, HR, W)
            remote(TP.at[g, 1 - b], PR.at[g], p_send.at[0], p_recv.at[g], fs_0=twin).start()

    def scatter(k, carry):
        remote(ZS.at[k], ZR.at[k], z_send.at[0], z_recv.at[0], fs_0=z_target(k)).start()
        return carry

    def sum_twin(g):
        with jax.named_scope(f"p08_t{g}"):
            remote(PR.at[g], PR.at[g], p_send.at[0], p_recv.at[g], fs_0=twin).wait_recv()
            part = TP[g, b] + PR[g]
            for e in range(E):
                ZS[g * E + e] = part[2 * e : 2 * e + 2]
            if g == 0:
                pl.semaphore_wait(ready.at[1], 2)
            lax.fori_loop(g * E, min((g + 1) * E, NP - 1), scatter, 0)

    for g in range(NG):
        sum_x(g)
        if g > 0:
            sum_twin(g - 1)
    sum_twin(NG - 1)
    with jax.named_scope("p09_zwait"):
        all_in = remote(ZR, ZR, z_send.at[0], z_recv.at[0], fs_0=next_z)
        all_in.wait_recv()
    with jax.named_scope("p10_moment"):
        proj = ZS[NP - 1] + jnp.sum(ZR[...], axis=0)
        give_m.wait_recv()

        def both(own, got):
            top = jnp.where(c == 0, own, got)
            low = jnp.where(c == 0, got, own)
            return jnp.concatenate([top, low], axis=0)

        moment = both(MS[c, 0], MR[0])
        square = both(MS[c, 1], MR[1])
        first = first_decay * moment + (1.0 - first_decay) * proj
        second = second_decay * square + (1.0 - second_decay) * proj * proj
        heading = first / (jnp.sqrt(second) + divide_guard)
        ZG[NP - 1] = heading

    def slot_of(k):
        return jnp.where(k == 0, 0, k + 2 * lax.rem(k, 2) - 1)

    def spread(k, carry):
        slot = slot_of(k)
        remote(ZG.at[NP - 1], ZG.at[slot], z_send.at[1], g_recv.at[lax.div(slot, E)], fs_0=z_target(k)).start()
        return carry

    with jax.named_scope("p11_zsend"):
        lax.fori_loop(0, NP - 1, spread, 0)

    with jax.named_scope("p12_squares"):
        wide = heading * heading
        row = wide[:, 0:128]
        for k in range(128, W, 128):
            row = row + wide[:, k : k + 128]
        QY[0] = jnp.sum(row, axis=0, keepdims=True)
        for d in range(1, ny):
            remote(QY.at[0], QY.at[d], q_send.at[0], q_recv.at[0], tp=lax.rem(y + d, ny)).start()

        out_fs[c, 0] = jnp.where(c == 0, first[0:1], first[1:2])
        out_fs[c, 1] = jnp.where(c == 0, second[0:1], second[1:2])
        FO[0] = jnp.where(c == 0, first[1:2], first[0:1])
        FO[1] = jnp.where(c == 0, second[1:2], second[0:1])
        give_f = remote(FO, out_fs.at[c], core_send.at[NG + 1], core_recv.at[NG + 1], fs_2=other)
        give_f.start()
        start = pl.multiple_of((z * nx + x) * 16, 16)
        factor = dot_t(F[c, pl.ds(start, 16), :], perm)
        if ny > 1:
            y_all = remote(
                QY.at[pl.ds(1, ny - 1)], QY.at[pl.ds(1, ny - 1)], q_send.at[0], q_recv.at[0], fs_0=next_z
            )
            y_all.wait_recv()
        QZ[NP - 1] = jnp.sum(QY[...], axis=0)

        def spread_q(k, carry):
            remote(QZ.at[NP - 1], QZ.at[slot_of(k)], q_send.at[1], q_recv.at[1], fs_0=z_target(k)).start()
            return carry

        lax.fori_loop(0, NP - 1, spread_q, 0)

    def to_x(g, parity):
        for d in x_order:
            t = lax.rem(x + d, nx)
            remote(HX.at[g, x, parity], HX.at[g, x, parity], h_send.at[0], h_recv.at[g], fs_1=t).start()

    def forward(g):
        with jax.named_scope(f"p13_z{g}"):
            count = min((g + 1) * E, NP - 1) - g * E
            if count:
                remote(
                    ZR.at[pl.ds(0, count)], ZR.at[pl.ds(0, count)], z_send.at[1], g_recv.at[g], fs_0=next_z
                ).wait_recv()
        for e in range(E):
            HX[g, x, b, 2 * e : 2 * e + 2] = ZG[g * E + e]
        remote(HX.at[g, x, b], HX.at[g, x, b], p_send.at[1], p_recv.at[NG + g], fs_0=twin).start()
        to_x(g, b)

    def forward_twin(g):
        with jax.named_scope(f"p14_t{g}"):
            remote(PR.at[g], PR.at[g], p_send.at[1], p_recv.at[NG + g], fs_0=twin).wait_recv()
        to_x(g, 1 - b)

    block = jnp.zeros((16, W), jnp.float32)

    def times(g, block):
        with jax.named_scope(f"p15_x{g}"):
            remote(XR.at[g], XR.at[g], h_send.at[0], h_recv.at[g], fs_1=next_x).wait_recv()
        return block + jnp.dot(
            factor[:, g * nx * GR : (g + 1) * nx * GR], HX[g].reshape(nx * GR, W),
            precision=lax.Precision.HIGHEST, preferred_element_type=jnp.float32,
        )

    order = list(reversed(range(NG)))
    for i, g in enumerate(order):
        forward(g)
        if i > 0:
            forward_twin(order[i - 1])
    with jax.named_scope("p16_q"):
        z_told = remote(
            QZ.at[pl.ds(0, NP - 1)], QZ.at[pl.ds(0, NP - 1)], q_send.at[1], q_recv.at[1], fs_0=next_z
        )
        z_told.wait_recv()
        QP[0] = jnp.sum(QZ[...], axis=0)

        def tell(j, carry):
            remote(QP.at[0], QP.at[j], q_send.at[2], q_recv.at[2], **around(j)).start()
            return carry

        lax.fori_loop(1, 4 * nx, tell, 0)
    forward_twin(order[-1])
    for g in order:
        block = times(g, block)
    ST[...] = block.reshape(2, 8, W)
    give_s = remote(ST.at[other], out_step.at[c], core_send.at[NG + 2], core_recv.at[NG + 2], fs_2=other)
    give_s.start()
    out_step[c] = ST[c]
    with jax.named_scope("p17_q"):
        told = QP.at[pl.ds(1, 4 * nx - 1)]
        q_all = remote(told, told, q_send.at[2], q_recv.at[2], fs_1=next_x)
        q_all.wait_recv()
        out_q[c] = jnp.sum(QP[0 : 2 * nx], axis=0)
        out_q[other] = jnp.sum(QP[2 * nx : 4 * nx], axis=0)

    with jax.named_scope("p18_drain"):
        for cp in (*give, give_m):
            cp.wait_send()
        remote(XR, XR, x_send.at[0], x_recv.at[0], fs_1=next_x).wait_send()
        for k in range(2):
            remote(PR, PR, p_send.at[k], p_recv.at[0], fs_0=twin).wait_send()
        all_in.wait_send()
        remote(ZR, ZR, z_send.at[1], g_recv.at[0], fs_0=next_z).wait_send()
        remote(XR, XR, h_send.at[0], h_recv.at[0], fs_1=next_x).wait_send()
        if ny > 1:
            y_all.wait_send()
        z_told.wait_send()
        q_all.wait_send()
        give_f.wait()
        give_s.wait()


def finish(entries, step, fs, q, mi, mo, fi, fo, si, so, ti, to, wi, wo, ci, co):
    fi[...] = fs[0, 0]
    si[...] = fs[0, 1]
    fo[...] = fs[1, 0]
    so[...] = fs[1, 1]
    for m, (old, out, new, copy) in enumerate(((mi, ti, wi, ci), (mo, to, wo, co))):
        mean = jnp.sum(q[m], axis=1, keepdims=True) / entries
        gain = jnp.minimum(1.0, clip_level / jnp.sqrt(mean + mean_guard))
        s = gain * step[m]
        out[...] = s
        w = old[...] - s
        new[...] = w
        copy[...] = w.astype(jnp.bfloat16)


def shards(nz, nx, ny, saved, unit, gated, mixer, left, right, mi, mo, m0, m1, s0, s1):
    f32, bf16 = jnp.float32, jnp.bfloat16
    n, d = saved.shape
    W = unit.shape[1]
    rank = left.shape[1]
    assert rank == 2 * nz * nx and nx == 4 and mi.shape[0] == 8 and m0.shape[0] == 1
    entries = float(rank * W * ny)
    V = pltpu.VMEM
    dma = pltpu.SemaphoreType.DMA
    NG, NP = groups_of(nz), nz // 2
    HR = 2 * NP // NG
    GR = 2 * HR
    anywhere = pl.BlockSpec(memory_space=pl.ANY)
    vmem = pl.BlockSpec(memory_space=pltpu.VMEM)
    step, fs, q = pl.pallas_call(
        functools.partial(exchange, nz, nx, ny),
        out_shape=(
            jax.ShapeDtypeStruct((2, 8, W), f32),
            jax.ShapeDtypeStruct((2, 2, 1, W), f32),
            jax.ShapeDtypeStruct((2, 1, 128), f32),
        ),
        in_specs=[anywhere] * 10,
        out_specs=(vmem, vmem, vmem),
        scratch_shapes=[
            V((2, 2, n // 2, d), bf16),
            V((2, d, rank), bf16),
            V((2, n, W), bf16),
            V((2, NG, nx * GR, W), f32),
            V((NG, nx * GR, W), f32),
            V((NG, nx, GR, W), f32),
            V((NG, nx - 1, GR, W), f32),
            V((NG, 2, HR, W), f32),
            V((NG, HR, W), f32),
            V((NP, 2, W), f32),
            V((NP - 1, 2, W), f32),
            V((NP, 2, W), f32),
            V((NG, nx, 2, HR, W), f32),
            V((2, 2, 1, W), f32),
            V((2, 1, W), f32),
            V((2, 1, W), f32),
            V((ny, 1, 128), f32),
            V((NP, 1, 128), f32),
            V((4 * nx, 1, 128), f32),
            V((2, 8, W), f32),
            dma((2, 4)),
            dma((4,)),
            dma((NG + 3,)),
            dma((NG + 3,)),
            dma((1,)),
            dma((NG,)),
            dma((2,)),
            dma((2 * NG,)),
            dma((2,)),
            dma((1,)),
            dma((NG,)),
            dma((1,)),
            dma((NG,)),
            dma((3,)),
            dma((3,)),
            pltpu.SemaphoreType.REGULAR((2,)),
        ],
        compiler_params=pltpu.CompilerParams(collective_id=0, has_side_effects=True),
        name="exchange",
    )(saved, unit, gated, mixer, left, right, m0, m1, s0, s1)
    row = jax.ShapeDtypeStruct((1, W), f32)
    wide = jax.ShapeDtypeStruct((8, W), f32)
    short = jax.ShapeDtypeStruct((8, W), bf16)
    outs = pl.pallas_call(
        functools.partial(finish, entries),
        out_shape=(row, row, row, row, wide, wide, wide, wide, short, short),
        name="finish",
    )(step, fs, q, mi, mo.T)
    return tuple(out.T if k in (5, 7, 9) else out for k, out in enumerate(outs))


def solution(mesh):
    ny = mesh.shape["tp"]
    nx = 4
    nz = mesh.shape["fs"] // (2 * nx)
    finer = Mesh(mesh.devices.reshape(nz, nx, 2, ny), (*FS, "tp"))
    rows, cols = P(FS, "tp"), P("tp", FS)
    return jax.shard_map(
        functools.partial(shards, nz, nx, ny),
        mesh=finer,
        in_specs=(P(FS, None), rows, rows, P(FS, None), P(), P(), rows, cols, rows, rows, rows, rows),
        out_specs=(rows, rows, rows, rows, rows, cols, rows, cols, rows, cols),
        check_vma=False,
    )
```

```python
import functools

import jax
import jax.numpy as jnp
from jax import lax
from jax.experimental import pallas as pl
from jax.experimental.pallas import tpu as pltpu
from jax.sharding import Mesh
from jax.sharding import PartitionSpec as P

FS = ("fs_0", "fs_1", "fs_2")
MESH = pl.DeviceIdType.MESH

first_decay = 0.9
second_decay = 0.95
divide_guard = 1e-08
mean_guard = 1e-06
clip_level = 0.1


def groups_of(nz):
    return min(4, nz // 2)


def permutation(nz, nx, base):
    n = 2 * nz * nx
    pairs = nz // 2
    E = pairs // groups_of(nz)
    p = lax.broadcasted_iota(jnp.int32, (n, n), 0)
    r = lax.broadcasted_iota(jnp.int32, (n, n), 1)
    log = lambda v: v.bit_length() - 1
    shift, mask = lax.shift_right_logical, lax.bitwise_and
    k = shift(p, log(4 * E * nx)) * E + mask(shift(p, 1), E - 1)
    parity = mask(shift(p, log(2 * E)), 1)
    px = mask(shift(p, log(4 * E)), nx - 1)
    reach = pairs // 2 - shift(k + 1, 1)
    offset = jnp.where(mask(k, 1) == 1, reach, -reach)
    target = mask(base + nz + 2 * offset + parity, nz - 1)
    want = target * (2 * nx) + 2 * px + mask(p, 1)
    return jnp.where(want == r, 1.0, 0.0).astype(jnp.bfloat16)


def dot_t(a, b):
    return lax.dot_general(a, b, (((1,), (1,)), ((), ())), preferred_element_type=jnp.float32)


def exchange(
    nz, nx, ny,
    a0, u0, u1, a1, l0, l1, m0, m1, s0, s1, w0, w1,
    out_step, out_fs, out_q, out_old,
    X, F, FP, RW, U, PS, CR, S, XR, TP, PR, ZS, ZR, ZG, HX, MS, MR, FO, QP, ST, FC,
    load_sem, small_sem, core_send, core_recv, x_send, x_recv, p_send, p_recv,
    z_send, z_recv, g_recv, h_send, h_recv, q_send, q_recv, ready,
):
    z = lax.axis_index("fs_0")
    x = lax.axis_index("fs_1")
    c = lax.axis_index("fs_2")
    y = lax.axis_index("tp")
    other = 1 - c
    W = u0.shape[1]
    tokens = a0.shape[0] // 2
    NG = groups_of(nz)
    NP = nz // 2
    E = NP // NG
    HR = 2 * E
    GR = 2 * HR
    b = lax.rem(z, 2)
    base = z - b
    twin = base + 1 - b
    reach = max(2, nz // 8)

    def z_at(offset):
        return lax.rem(z + nz + offset, nz)

    def z_target(k):
        far = NP // 2 - (k + 1) // 2
        return z_at(2 * far * (2 * (k % 2) - 1))

    def around(j):
        return {
            "fs_0": base + lax.rem(b + lax.rem(lax.div(j, nx), 2), 2),
            "fs_1": lax.rem(x + lax.rem(j, nx), nx),
            "fs_2": lax.rem(c + lax.div(j, 2 * nx), 2),
        }

    with jax.named_scope("p00_loads"):
        sources = ((l0, a0, u0), (l1, a1, u1))
        halves = (pl.ds(0, tokens), pl.ds(tokens, tokens))

        def parts(m):
            l, a, u = sources[m]
            return (
                (l, F.at[m]), (a.at[halves[0]], X.at[m, 0]), (a.at[halves[1]], X.at[m, 1]), (u, U.at[m]),
            )

        for mine in range(2):

            @pl.when(c == mine)
            def _(mine=mine):
                for m, k in [(m, k) for ks in ((0,), (1, 2, 3)) for m in (1 - mine, mine) for k in ks]:
                    src, dst = parts(m)[k]
                    pltpu.make_async_copy(src, dst, load_sem.at[m, k]).start()

        small = []
        for k, (src, dst) in enumerate((
            (m0, MS.at[0, 0]), (s0, MS.at[0, 1]), (m1, MS.at[1, 0]), (s1, MS.at[1, 1]), (w0, out_old.at[0]), (w1, out_old.at[1]),
        )):
            cp = pltpu.make_async_copy(src, dst, small_sem.at[k])
            cp.start()
            small.append(cp)

    with jax.named_scope("p01_greet"):
        barrier = pltpu.get_barrier_semaphore()
        met = 0
        for d in range(reach, 0, -2):
            for offset in (d, -d):
                pl.semaphore_signal(barrier, inc=1, device_id={"fs_0": z_at(offset)}, device_id_type=MESH)
                met += 1
        for d in range(1, ny):
            pl.semaphore_signal(barrier, inc=1, device_id={"tp": lax.rem(y + d, ny)}, device_id_type=MESH)
            met += 1

        def greet(j, carry):
            pl.semaphore_signal(barrier, inc=1, device_id=around(j), device_id_type=MESH)
            return carry

        lax.fori_loop(1, 4 * nx, greet, 0)
        met += 4 * nx - 1

    perm = permutation(nz, nx, base)

    def arrived(m, k):
        src, dst = parts(0)[k]
        dst = (F.at[m], X.at[m, 0], X.at[m, 1], U.at[m])[k]
        pltpu.make_async_copy(src, dst, load_sem.at[m, k]).wait()

    def project(m):
        for h in range(2):
            arrived(m, 1 + h)
            RW[halves[h]] = jnp.dot(X[m, h], FP[m], preferred_element_type=jnp.float32).astype(jnp.bfloat16)
        arrived(m, 3)
        sums = lax.dot_general(
            RW[...], U[m], (((0,), (0,)), ((), ())), preferred_element_type=jnp.float32
        )
        PS[m] = sums.reshape(NG, nx * GR, W)

    def remote(src, dst, send, recv, **where):
        return pltpu.make_async_remote_copy(
            src_ref=src, dst_ref=dst, send_sem=send, recv_sem=recv, device_id=where, device_id_type=MESH
        )

    with jax.named_scope("p02_factors"):
        for m in (other, c):
            arrived(m, 0)
            FP[m] = dot_t(F[m], perm).astype(jnp.bfloat16)
    with jax.named_scope("p02_project"):
        project(other)
        for cp in small:
            cp.wait()
    with jax.named_scope("p03_barrier"):
        pl.semaphore_wait(barrier, met)

    for offset in (reach, -reach):
        pl.semaphore_signal(ready.at[0], inc=1, device_id={"fs_0": z_at(offset)}, device_id_type=MESH)
    for d in range(1, ny):
        pl.semaphore_signal(ready.at[0], inc=1, device_id={"tp": lax.rem(y + d, ny)}, device_id_type=MESH)

    give = [
        remote(PS.at[other, g], CR.at[g], core_send.at[g], core_recv.at[g], fs_2=other) for g in range(NG)
    ]
    for cp in give:
        cp.start()
    give_m = remote(MS.at[other], MR, core_send.at[NG], core_recv.at[NG], fs_2=other)
    give_m.start()
    with jax.named_scope("p04_project"):
        project(c)

    x_order = (2, 1, 3)
    with jax.named_scope("p05_xsend"):
        for g in range(NG):
            give[g].wait_recv()
            S[g] = (PS[c, g] + CR[g]).reshape(nx, GR, W)
            for d in x_order:
                t = lax.rem(x + d, nx)
                remote(S.at[g, t], XR.at[g, d - 1], x_send.at[0], x_recv.at[g], fs_1=t).start()

    with jax.named_scope("p06_ready"):
        pl.semaphore_wait(ready.at[0], 1 + ny)
        for offset in (2 * reach, -2 * reach):
            pl.semaphore_signal(ready.at[1], inc=1, device_id={"fs_0": z_at(offset)}, device_id_type=MESH)

    next_x = lax.rem(x + 1, nx)
    next_z = z_at(2)

    def sum_x(g):
        with jax.named_scope(f"p07_x{g}"):
            remote(XR.at[g], XR.at[g], x_send.at[0], x_recv.at[g], fs_1=next_x).wait_recv()
            part = S[g, x] + (XR[g, 0] + XR[g, 1] + XR[g, 2])
            TP[g] = part.reshape(2, HR, W)
            remote(TP.at[g, 1 - b], PR.at[g], p_send.at[0], p_recv.at[g], fs_0=twin).start()

    def sum_twin(g):
        with jax.named_scope(f"p08_t{g}"):
            remote(PR.at[g], PR.at[g], p_send.at[0], p_recv.at[g], fs_0=twin).wait_recv()
            part = TP[g, b] + PR[g]
            for e in range(E):
                ZS[g * E + e] = part[2 * e : 2 * e + 2]
            if g == 0:
                pl.semaphore_wait(ready.at[1], 2)
            for k in range(g * E, min((g + 1) * E, NP - 1)):
                remote(ZS.at[k], ZR.at[k], z_send.at[0], z_recv.at[0], fs_0=z_target(k)).start()

    for g in range(NG):
        sum_x(g)
        if g > 0:
            sum_twin(g - 1)
    sum_twin(NG - 1)
    with jax.named_scope("p09_zwait"):
        all_in = remote(ZR, ZR, z_send.at[0], z_recv.at[0], fs_0=next_z)
        all_in.wait_recv()
    with jax.named_scope("p10_moment"):
        proj = ZS[NP - 1] + jnp.sum(ZR[...], axis=0)
        give_m.wait_recv()

        def both(own, got):
            top = jnp.where(c == 0, own, got)
            low = jnp.where(c == 0, got, own)
            return jnp.concatenate([top, low], axis=0)

        moment = both(MS[c, 0], MR[0])
        square = both(MS[c, 1], MR[1])
        first = first_decay * moment + (1.0 - first_decay) * proj
        second = second_decay * square + (1.0 - second_decay) * proj * proj
        heading = first / (jnp.sqrt(second) + divide_guard)
        ZG[NP - 1] = heading

    with jax.named_scope("p11_zsend"):
        for k in range(NP - 1):
            slot = k + 2 * (k % 2) - 1 if k else 0
            remote(ZG.at[NP - 1], ZG.at[slot], z_send.at[1], g_recv.at[slot // E], fs_0=z_target(k)).start()

    with jax.named_scope("p12_owner"):
        out_fs[c, 0] = jnp.where(c == 0, first[0:1], first[1:2])
        out_fs[c, 1] = jnp.where(c == 0, second[0:1], second[1:2])
        FO[0] = jnp.where(c == 0, first[1:2], first[0:1])
        FO[1] = jnp.where(c == 0, second[1:2], second[0:1])
        give_f = remote(FO, out_fs.at[c], core_send.at[NG + 1], core_recv.at[NG + 1], fs_2=other)
        give_f.start()
        start = pl.multiple_of((z * nx + x) * 16, 16)
        factor = FP[c, pl.ds(start, 16), :]
        for g in range(NG):
            FC[g] = factor[:, g * nx * GR : (g + 1) * nx * GR]

    def to_x(g, parity):
        for d in x_order:
            t = lax.rem(x + d, nx)
            remote(HX.at[g, x, parity], HX.at[g, x, parity], h_send.at[0], h_recv.at[g], fs_1=t).start()

    def forward(g, squares):
        with jax.named_scope(f"p13_z{g}"):
            count = min((g + 1) * E, NP - 1) - g * E
            if count:
                remote(
                    ZR.at[pl.ds(0, count)], ZR.at[pl.ds(0, count)], z_send.at[1], g_recv.at[g], fs_0=next_z
                ).wait_recv()
        for e in range(E):
            piece = ZG[g * E + e]
            HX[g, x, b, 2 * e : 2 * e + 2] = piece
            piece = piece * piece
            for k in range(0, W, 128):
                squares = squares + piece[:, k : k + 128]
        remote(HX.at[g, x, b], HX.at[g, x, b], p_send.at[1], p_recv.at[NG + g], fs_0=twin).start()
        to_x(g, b)
        if g == 0:
            for d in x_order:
                t = lax.rem(x + d, nx)
                remote(
                    HX.at[g, x, b], HX.at[g, x, b], h_send.at[0], h_recv.at[g], fs_0=twin, fs_1=t
                ).start()
            QP[0] = jnp.sum(squares, axis=0, keepdims=True)
            tell()
        return squares

    crowd = 4 * nx * ny

    def tell():
        sides = [lax.rem(x + d, nx) for d in range(nx)]
        ups = [lax.rem(y + d, ny) for d in range(ny)]
        for dy in sorted(range(ny), key=lambda d: -min(d, ny - d)):
            for dx in sorted(range(nx), key=lambda d: -min(d, nx - d)):
                for db in (1, 0):
                    for dc in (1, 0):
                        slot = dc * (crowd // 2) + (db * ny + dy) * nx + dx
                        if slot:
                            remote(
                                QP.at[0], QP.at[slot], q_send.at[0], q_recv.at[0],
                                fs_0=(z, twin)[db], fs_1=sides[dx], fs_2=(c, other)[dc], tp=ups[dy],
                            ).start()

    def forward_twin(g):
        with jax.named_scope(f"p14_t{g}"):
            remote(PR.at[g], PR.at[g], p_send.at[1], p_recv.at[NG + g], fs_0=twin).wait_recv()
        if g > 0:
            to_x(g, 1 - b)

    squares = jnp.zeros((2, 128), jnp.float32)
    for g in reversed(range(NG)):
        squares = forward(g, squares)
        if g < NG - 1:
            forward_twin(g + 1)
    forward_twin(0)

    def times(i, block):
        g = NG - 1 - i
        remote(XR.at[g], XR.at[g], h_send.at[0], h_recv.at[g], fs_1=next_x).wait_recv()
        whole = HX[g].reshape(nx * GR, W)
        high = whole.astype(jnp.bfloat16)
        rest = whole - high.astype(jnp.float32)
        middle = rest.astype(jnp.bfloat16)
        low = (rest - middle.astype(jnp.float32)).astype(jnp.bfloat16)
        part = FC[g]
        return block + jnp.dot(
            jnp.concatenate([part, part, part], axis=1), jnp.concatenate([low, middle, high], axis=0),
            preferred_element_type=jnp.float32,
        )

    with jax.named_scope("p15_x"):
        block = lax.fori_loop(0, NG, times, jnp.zeros((16, W), jnp.float32))
    ST[...] = block.reshape(2, 8, W)
    give_s = remote(ST.at[other], out_step.at[c], core_send.at[NG + 2], core_recv.at[NG + 2], fs_2=other)
    give_s.start()
    out_step[c] = ST[c]
    with jax.named_scope("p17_q"):
        told = QP.at[pl.ds(1, crowd - 1)]
        q_all = remote(told, told, q_send.at[0], q_recv.at[0], fs_1=next_x)
        q_all.wait_recv()
        out_q[c] = jnp.sum(QP[0 : crowd // 2], axis=0)
        out_q[other] = jnp.sum(QP[crowd // 2 : crowd], axis=0)

    with jax.named_scope("p18_drain"):
        for cp in (*give, give_m):
            cp.wait_send()
        remote(XR, XR, x_send.at[0], x_recv.at[0], fs_1=next_x).wait_send()
        for k in range(2):
            remote(PR, PR, p_send.at[k], p_recv.at[0], fs_0=twin).wait_send()
        all_in.wait_send()
        remote(ZR, ZR, z_send.at[1], g_recv.at[0], fs_0=next_z).wait_send()
        remote(XR, XR, h_send.at[0], h_recv.at[0], fs_1=next_x).wait_send()
        q_all.wait_send()
        give_f.wait()
        give_s.wait()


def finish(entries, step, fs, q, old, fi, fo, si, so, ti, to, wi, wo, ci, co):
    fi[...] = fs[0, 0]
    si[...] = fs[0, 1]
    fo[...] = fs[1, 0]
    so[...] = fs[1, 1]
    for m, (out, new, copy) in enumerate(((ti, wi, ci), (to, wo, co))):
        mean = jnp.sum(q[m], axis=1, keepdims=True) / entries
        gain = jnp.minimum(1.0, clip_level / jnp.sqrt(mean + mean_guard))
        s = gain * step[m]
        out[...] = s
        w = old[m] - s
        new[...] = w
        copy[...] = w.astype(jnp.bfloat16)


def shards(nz, nx, ny, saved, unit, gated, mixer, left, right, mi, mo, m0, m1, s0, s1):
    f32, bf16 = jnp.float32, jnp.bfloat16
    n, d = saved.shape
    W = unit.shape[1]
    rank = left.shape[1]
    assert rank == 2 * nz * nx and nx == 4 and mi.shape[0] == 8 and m0.shape[0] == 1
    entries = float(rank * W * ny)
    V = pltpu.VMEM
    dma = pltpu.SemaphoreType.DMA
    NG, NP = groups_of(nz), nz // 2
    HR = 2 * NP // NG
    GR = 2 * HR
    anywhere = pl.BlockSpec(memory_space=pl.ANY)
    vmem = pl.BlockSpec(memory_space=pltpu.VMEM)
    step, fs, q, old = pl.pallas_call(
        functools.partial(exchange, nz, nx, ny),
        out_shape=(
            V((2, 8, W), f32),
            V((2, 2, 1, W), f32),
            V((2, 1, 128), f32),
            V((2, 8, W), f32),
        ),
        in_specs=[anywhere] * 12,
        out_specs=(vmem, vmem, vmem, vmem),
        scratch_shapes=[
            V((2, 2, n // 2, d), bf16),
            V((2, d, rank), bf16),
            V((2, d, rank), bf16),
            V((n, rank), bf16),
            V((2, n, W), bf16),
            V((2, NG, nx * GR, W), f32),
            V((NG, nx * GR, W), f32),
            V((NG, nx, GR, W), f32),
            V((NG, nx - 1, GR, W), f32),
            V((NG, 2, HR, W), f32),
            V((NG, HR, W), f32),
            V((NP, 2, W), f32),
            V((NP - 1, 2, W), f32),
            V((NP, 2, W), f32),
            V((NG, nx, 2, HR, W), f32),
            V((2, 2, 1, W), f32),
            V((2, 1, W), f32),
            V((2, 1, W), f32),
            V((4 * nx * ny, 1, 128), f32),
            V((2, 8, W), f32),
            V((NG, 16, nx * GR), bf16),
            dma((2, 4)),
            dma((6,)),
            dma((NG + 3,)),
            dma((NG + 3,)),
            dma((1,)),
            dma((NG,)),
            dma((2,)),
            dma((2 * NG,)),
            dma((2,)),
            dma((1,)),
            dma((NG,)),
            dma((1,)),
            dma((NG,)),
            dma((1,)),
            dma((1,)),
            pltpu.SemaphoreType.REGULAR((2,)),
        ],
        compiler_params=pltpu.CompilerParams(collective_id=0, has_side_effects=True),
        name="exchange",
    )(saved, unit, gated, mixer, left, right, m0, m1, s0, s1, mi, mo.T)
    row = jax.ShapeDtypeStruct((1, W), f32)
    wide = jax.ShapeDtypeStruct((8, W), f32)
    short = jax.ShapeDtypeStruct((8, W), bf16)
    outs = pl.pallas_call(
        functools.partial(finish, entries),
        out_shape=(row, row, row, row, wide, wide, wide, wide, short, short),
        in_specs=[vmem] * 4,
        name="finish",
    )(*(pltpu.with_memory_space_constraint(v, pltpu.VMEM) for v in (step, fs, q, old)))
    return tuple(out.T if k in (5, 7, 9) else out for k, out in enumerate(outs))


def solution(mesh):
    ny = mesh.shape["tp"]
    nx = 4
    nz = mesh.shape["fs"] // (2 * nx)
    finer = Mesh(mesh.devices.reshape(nz, nx, 2, ny), (*FS, "tp"))
    rows, cols = P(FS, "tp"), P("tp", FS)
    return jax.shard_map(
        functools.partial(shards, nz, nx, ny),
        mesh=finer,
        in_specs=(P(FS, None), rows, rows, P(FS, None), P(), P(), rows, cols, rows, rows, rows, rows),
        out_specs=(rows, rows, rows, rows, rows, cols, rows, cols, rows, cols),
        check_vma=False,
    )
```

```python
import functools

import jax
import jax.numpy as jnp
from jax import lax
from jax.experimental import pallas as pl
from jax.experimental.pallas import tpu as pltpu
from jax.sharding import Mesh
from jax.sharding import PartitionSpec as P

FS = ("fs_0", "fs_1", "fs_2")
MESH = pl.DeviceIdType.MESH

first_decay = 0.9
second_decay = 0.95
divide_guard = 1e-08
mean_guard = 1e-06
clip_level = 0.1


def groups_of(nz):
    return min(4, nz // 2)


def permutation(nz, nx, base):
    n = 2 * nz * nx
    pairs = nz // 2
    E = pairs // groups_of(nz)
    p = lax.broadcasted_iota(jnp.int32, (n, n), 0)
    r = lax.broadcasted_iota(jnp.int32, (n, n), 1)
    log = lambda v: v.bit_length() - 1
    shift, mask = lax.shift_right_logical, lax.bitwise_and
    k = shift(p, log(4 * E * nx)) * E + mask(shift(p, 1), E - 1)
    parity = mask(shift(p, log(2 * E)), 1)
    px = mask(shift(p, log(4 * E)), nx - 1)
    reach = pairs // 2 - shift(k + 1, 1)
    offset = jnp.where(mask(k, 1) == 1, reach, -reach)
    target = mask(base + nz + 2 * offset + parity, nz - 1)
    want = target * (2 * nx) + 2 * px + mask(p, 1)
    return jnp.where(want == r, 1.0, 0.0).astype(jnp.bfloat16)


def dot_t(a, b):
    return lax.dot_general(a, b, (((1,), (1,)), ((), ())), preferred_element_type=jnp.float32)


def exchange(
    nz, nx, ny,
    a0, u0, u1, a1, l0, l1, m0, m1, s0, s1, w0, w1,
    out_step, out_fs, out_q, out_old,
    X, F, FP, RW, U, PS, CR, S, XR, TP, PR, ZS, ZR, ZG, HX, MS, MR, FO, QP, ST, FC,
    load_sem, small_sem, core_send, core_recv, x_send, x_recv, p_send, p_recv,
    z_send, z_recv, g_recv, h_send, h_recv, q_send, q_recv, ready,
):
    z = lax.axis_index("fs_0")
    x = lax.axis_index("fs_1")
    c = lax.axis_index("fs_2")
    y = lax.axis_index("tp")
    other = 1 - c
    W = u0.shape[1]
    tokens = a0.shape[0] // 2
    NG = groups_of(nz)
    NP = nz // 2
    E = NP // NG
    HR = 2 * E
    GR = 2 * HR
    b = lax.rem(z, 2)
    base = z - b
    twin = base + 1 - b
    reach = max(2, nz // 8)

    def z_at(offset):
        return lax.rem(z + nz + offset, nz)

    def z_target(k):
        far = NP // 2 - (k + 1) // 2
        return z_at(2 * far * (2 * (k % 2) - 1))

    def around(j):
        return {
            "fs_0": base + lax.rem(b + lax.rem(lax.div(j, nx), 2), 2),
            "fs_1": lax.rem(x + lax.rem(j, nx), nx),
            "fs_2": lax.rem(c + lax.div(j, 2 * nx), 2),
        }

    with jax.named_scope("p00_loads"):
        sources = ((l0, a0, u0), (l1, a1, u1))
        halves = (pl.ds(0, tokens), pl.ds(tokens, tokens))

        def parts(m):
            l, a, u = sources[m]
            return (
                (l, F.at[m]), (a.at[halves[0]], X.at[m, 0]), (a.at[halves[1]], X.at[m, 1]), (u, U.at[m]),
            )

        for mine in range(2):

            @pl.when(c == mine)
            def _(mine=mine):
                for m, k in [(m, k) for ks in ((0,), (1, 2, 3)) for m in (1 - mine, mine) for k in ks]:
                    src, dst = parts(m)[k]
                    pltpu.make_async_copy(src, dst, load_sem.at[m, k]).start()

        small = []
        for k, (src, dst) in enumerate((
            (m0, MS.at[0, 0]), (s0, MS.at[0, 1]), (m1, MS.at[1, 0]), (s1, MS.at[1, 1]), (w0, out_old.at[0]), (w1, out_old.at[1]),
        )):
            cp = pltpu.make_async_copy(src, dst, small_sem.at[k])
            cp.start()
            small.append(cp)

    with jax.named_scope("p01_greet"):
        barrier = pltpu.get_barrier_semaphore()
        met = 0
        for d in range(reach, 0, -2):
            for offset in (d, -d):
                pl.semaphore_signal(barrier, inc=1, device_id={"fs_0": z_at(offset)}, device_id_type=MESH)
                met += 1
        for d in range(1, ny):
            pl.semaphore_signal(barrier, inc=1, device_id={"tp": lax.rem(y + d, ny)}, device_id_type=MESH)
            met += 1

        def greet(j, carry):
            pl.semaphore_signal(barrier, inc=1, device_id=around(j), device_id_type=MESH)
            return carry

        lax.fori_loop(1, 4 * nx, greet, 0)
        met += 4 * nx - 1

    perm = permutation(nz, nx, base)

    def arrived(m, k):
        src, dst = parts(0)[k]
        dst = (F.at[m], X.at[m, 0], X.at[m, 1], U.at[m])[k]
        pltpu.make_async_copy(src, dst, load_sem.at[m, k]).wait()

    def project(m):
        for h in range(2):
            arrived(m, 1 + h)
            RW[halves[h]] = jnp.dot(X[m, h], FP[m], preferred_element_type=jnp.float32).astype(jnp.bfloat16)
        arrived(m, 3)
        sums = lax.dot_general(
            RW[...], U[m], (((0,), (0,)), ((), ())), preferred_element_type=jnp.float32
        )
        PS[m] = sums.reshape(NG, nx * GR, W)

    def remote(src, dst, send, recv, **where):
        return pltpu.make_async_remote_copy(
            src_ref=src, dst_ref=dst, send_sem=send, recv_sem=recv, device_id=where, device_id_type=MESH
        )

    with jax.named_scope("p02_factors"):
        for m in (other, c):
            arrived(m, 0)
            FP[m] = dot_t(F[m], perm).astype(jnp.bfloat16)
    with jax.named_scope("p02_project"):
        project(other)
        for cp in small:
            cp.wait()
    with jax.named_scope("p03_barrier"):
        pl.semaphore_wait(barrier, met)

    for offset in (reach, -reach):
        pl.semaphore_signal(ready.at[0], inc=1, device_id={"fs_0": z_at(offset)}, device_id_type=MESH)
    for d in range(1, ny):
        pl.semaphore_signal(ready.at[0], inc=1, device_id={"tp": lax.rem(y + d, ny)}, device_id_type=MESH)

    give = [
        remote(PS.at[other, g], CR.at[g], core_send.at[g], core_recv.at[g], fs_2=other) for g in range(NG)
    ]
    for cp in give:
        cp.start()
    give_m = remote(MS.at[other], MR, core_send.at[NG], core_recv.at[NG], fs_2=other)
    give_m.start()
    with jax.named_scope("p04_project"):
        project(c)

    x_order = (2, 1, 3)
    with jax.named_scope("p05_xsend"):
        for g in range(NG):
            give[g].wait_recv()
            S[g] = (PS[c, g] + CR[g]).reshape(nx, GR, W)
            for d in x_order:
                t = lax.rem(x + d, nx)
                remote(S.at[g, t], XR.at[g, d - 1], x_send.at[0], x_recv.at[g], fs_1=t).start()

    with jax.named_scope("p06_ready"):
        pl.semaphore_wait(ready.at[0], 1 + ny)
        for offset in (2 * reach, -2 * reach):
            pl.semaphore_signal(ready.at[1], inc=1, device_id={"fs_0": z_at(offset)}, device_id_type=MESH)

    next_x = lax.rem(x + 1, nx)
    next_z = z_at(2)

    def sum_x(g):
        with jax.named_scope(f"p07_x{g}"):
            remote(XR.at[g], XR.at[g], x_send.at[0], x_recv.at[g], fs_1=next_x).wait_recv()
            part = S[g, x] + (XR[g, 0] + XR[g, 1] + XR[g, 2])
            TP[g] = part.reshape(2, HR, W)
            remote(TP.at[g, 1 - b], PR.at[g], p_send.at[0], p_recv.at[g], fs_0=twin).start()

    def sum_twin(g):
        with jax.named_scope(f"p08_t{g}"):
            remote(PR.at[g], PR.at[g], p_send.at[0], p_recv.at[g], fs_0=twin).wait_recv()
            part = TP[g, b] + PR[g]
            for e in range(E):
                ZS[g * E + e] = part[2 * e : 2 * e + 2]
            if g == 0:
                pl.semaphore_wait(ready.at[1], 2)
            for k in range(g * E, min((g + 1) * E, NP - 1)):
                remote(ZS.at[k], ZR.at[k], z_send.at[0], z_recv.at[0], fs_0=z_target(k)).start()

    for g in range(NG):
        sum_x(g)
        if g > 0:
            sum_twin(g - 1)
    sum_twin(NG - 1)
    with jax.named_scope("p09_zwait"):
        all_in = remote(ZR, ZR, z_send.at[0], z_recv.at[0], fs_0=next_z)
        all_in.wait_recv()
    with jax.named_scope("p10_moment"):
        proj = ZS[NP - 1] + jnp.sum(ZR[...], axis=0)
        give_m.wait_recv()

        def both(own, got):
            top = jnp.where(c == 0, own, got)
            low = jnp.where(c == 0, got, own)
            return jnp.concatenate([top, low], axis=0)

        moment = both(MS[c, 0], MR[0])
        square = both(MS[c, 1], MR[1])
        first = first_decay * moment + (1.0 - first_decay) * proj
        second = second_decay * square + (1.0 - second_decay) * proj * proj
        heading = first / (jnp.sqrt(second) + divide_guard)
        ZG[NP - 1] = heading

    with jax.named_scope("p11_zsend"):
        for k in range(NP - 1):
            slot = k + 2 * (k % 2) - 1 if k else 0
            remote(ZG.at[NP - 1], ZG.at[slot], z_send.at[1], g_recv.at[slot // E], fs_0=z_target(k)).start()

    with jax.named_scope("p12_owner"):
        out_fs[c, 0] = jnp.where(c == 0, first[0:1], first[1:2])
        out_fs[c, 1] = jnp.where(c == 0, second[0:1], second[1:2])
        FO[0] = jnp.where(c == 0, first[1:2], first[0:1])
        FO[1] = jnp.where(c == 0, second[1:2], second[0:1])
        give_f = remote(FO, out_fs.at[c], core_send.at[NG + 1], core_recv.at[NG + 1], fs_2=other)
        give_f.start()
        start = pl.multiple_of((z * nx + x) * 16, 16)
        factor = FP[c, pl.ds(start, 16), :]
        for g in range(NG):
            FC[g] = factor[:, g * nx * GR : (g + 1) * nx * GR]

    def to_x(g, parity):
        for d in x_order:
            t = lax.rem(x + d, nx)
            remote(HX.at[g, x, parity], HX.at[g, x, parity], h_send.at[0], h_recv.at[g], fs_1=t).start()

    def forward(g, squares):
        with jax.named_scope(f"p13_z{g}"):
            count = min((g + 1) * E, NP - 1) - g * E
            if count:
                remote(
                    ZR.at[pl.ds(0, count)], ZR.at[pl.ds(0, count)], z_send.at[1], g_recv.at[g], fs_0=next_z
                ).wait_recv()
        for e in range(E):
            piece = ZG[g * E + e]
            piece = piece * piece
            for k in range(0, W, 128):
                squares = squares + piece[:, k : k + 128]
        if g == 0:
            QP[0] = jnp.sum(squares, axis=0, keepdims=True)
            tell()
        for e in range(E):
            HX[g, x, b, 2 * e : 2 * e + 2] = ZG[g * E + e]
        remote(HX.at[g, x, b], HX.at[g, x, b], p_send.at[1], p_recv.at[NG + g], fs_0=twin).start()
        to_x(g, b)
        if g == 0:
            for d in x_order:
                t = lax.rem(x + d, nx)
                remote(
                    HX.at[g, x, b], HX.at[g, x, b], h_send.at[0], h_recv.at[g], fs_0=twin, fs_1=t
                ).start()
        return squares

    crowd = 4 * nx * ny

    def tell():
        sides = [lax.rem(x + d, nx) for d in range(nx)]
        ups = [lax.rem(y + d, ny) for d in range(ny)]
        for dy in sorted(range(ny), key=lambda d: -min(d, ny - d)):
            for dx in sorted(range(nx), key=lambda d: -min(d, nx - d)):
                for db in (1, 0):
                    for dc in (1, 0):
                        slot = dc * (crowd // 2) + (db * ny + dy) * nx + dx
                        if slot:
                            remote(
                                QP.at[0], QP.at[slot], q_send.at[0], q_recv.at[0],
                                fs_0=(z, twin)[db], fs_1=sides[dx], fs_2=(c, other)[dc], tp=ups[dy],
                            ).start()

    def forward_twin(g):
        with jax.named_scope(f"p14_t{g}"):
            remote(PR.at[g], PR.at[g], p_send.at[1], p_recv.at[NG + g], fs_0=twin).wait_recv()
        if g > 0:
            to_x(g, 1 - b)

    squares = jnp.zeros((2, 128), jnp.float32)
    for g in reversed(range(NG)):
        squares = forward(g, squares)
        if g < NG - 1:
            forward_twin(g + 1)
    forward_twin(0)

    def times(i, block):
        g = NG - 1 - i
        remote(XR.at[g], XR.at[g], h_send.at[0], h_recv.at[g], fs_1=next_x).wait_recv()
        whole = HX[g].reshape(nx * GR, W)
        high = whole.astype(jnp.bfloat16)
        rest = whole - high.astype(jnp.float32)
        middle = rest.astype(jnp.bfloat16)
        low = (rest - middle.astype(jnp.float32)).astype(jnp.bfloat16)
        part = FC[g]
        return block + jnp.dot(
            jnp.concatenate([part, part, part], axis=1), jnp.concatenate([low, middle, high], axis=0),
            preferred_element_type=jnp.float32,
        )

    with jax.named_scope("p15_x"):
        block = lax.fori_loop(0, NG, times, jnp.zeros((16, W), jnp.float32))
    ST[...] = block.reshape(2, 8, W)
    give_s = remote(ST.at[other], out_step.at[c], core_send.at[NG + 2], core_recv.at[NG + 2], fs_2=other)
    give_s.start()
    out_step[c] = ST[c]
    with jax.named_scope("p17_q"):
        told = QP.at[pl.ds(1, crowd - 1)]
        q_all = remote(told, told, q_send.at[0], q_recv.at[0], fs_1=next_x)
        q_all.wait_recv()
        out_q[c] = jnp.sum(QP[0 : crowd // 2], axis=0)
        out_q[other] = jnp.sum(QP[crowd // 2 : crowd], axis=0)

    with jax.named_scope("p18_drain"):
        for cp in (*give, give_m):
            cp.wait_send()
        remote(XR, XR, x_send.at[0], x_recv.at[0], fs_1=next_x).wait_send()
        for k in range(2):
            remote(PR, PR, p_send.at[k], p_recv.at[0], fs_0=twin).wait_send()
        all_in.wait_send()
        remote(ZR, ZR, z_send.at[1], g_recv.at[0], fs_0=next_z).wait_send()
        remote(XR, XR, h_send.at[0], h_recv.at[0], fs_1=next_x).wait_send()
        q_all.wait_send()
        give_f.wait()
        give_s.wait()


def finish(entries, step, fs, q, old, fi, fo, si, so, ti, to, wi, wo, ci, co):
    fi[...] = fs[0, 0]
    si[...] = fs[0, 1]
    fo[...] = fs[1, 0]
    so[...] = fs[1, 1]
    for m, (out, new, copy) in enumerate(((ti, wi, ci), (to, wo, co))):
        mean = jnp.sum(q[m], axis=1, keepdims=True) / entries
        gain = jnp.minimum(1.0, clip_level / jnp.sqrt(mean + mean_guard))
        s = gain * step[m]
        out[...] = s
        w = old[m] - s
        new[...] = w
        copy[...] = w.astype(jnp.bfloat16)


def shards(nz, nx, ny, saved, unit, gated, mixer, left, right, mi, mo, m0, m1, s0, s1):
    f32, bf16 = jnp.float32, jnp.bfloat16
    n, d = saved.shape
    W = unit.shape[1]
    rank = left.shape[1]
    assert rank == 2 * nz * nx and nx == 4 and mi.shape[0] == 8 and m0.shape[0] == 1
    entries = float(rank * W * ny)
    V = pltpu.VMEM
    dma = pltpu.SemaphoreType.DMA
    NG, NP = groups_of(nz), nz // 2
    HR = 2 * NP // NG
    GR = 2 * HR
    anywhere = pl.BlockSpec(memory_space=pl.ANY)
    vmem = pl.BlockSpec(memory_space=pltpu.VMEM)
    step, fs, q, old = pl.pallas_call(
        functools.partial(exchange, nz, nx, ny),
        out_shape=(
            V((2, 8, W), f32),
            V((2, 2, 1, W), f32),
            V((2, 1, 128), f32),
            V((2, 8, W), f32),
        ),
        in_specs=[anywhere] * 12,
        out_specs=(vmem, vmem, vmem, vmem),
        scratch_shapes=[
            V((2, 2, n // 2, d), bf16),
            V((2, d, rank), bf16),
            V((2, d, rank), bf16),
            V((n, rank), bf16),
            V((2, n, W), bf16),
            V((2, NG, nx * GR, W), f32),
            V((NG, nx * GR, W), f32),
            V((NG, nx, GR, W), f32),
            V((NG, nx - 1, GR, W), f32),
            V((NG, 2, HR, W), f32),
            V((NG, HR, W), f32),
            V((NP, 2, W), f32),
            V((NP - 1, 2, W), f32),
            V((NP, 2, W), f32),
            V((NG, nx, 2, HR, W), f32),
            V((2, 2, 1, W), f32),
            V((2, 1, W), f32),
            V((2, 1, W), f32),
            V((4 * nx * ny, 1, 128), f32),
            V((2, 8, W), f32),
            V((NG, 16, nx * GR), bf16),
            dma((2, 4)),
            dma((6,)),
            dma((NG + 3,)),
            dma((NG + 3,)),
            dma((1,)),
            dma((NG,)),
            dma((2,)),
            dma((2 * NG,)),
            dma((2,)),
            dma((1,)),
            dma((NG,)),
            dma((1,)),
            dma((NG,)),
            dma((1,)),
            dma((1,)),
            pltpu.SemaphoreType.REGULAR((2,)),
        ],
        compiler_params=pltpu.CompilerParams(collective_id=0, has_side_effects=True),
        name="exchange",
    )(saved, unit, gated, mixer, left, right, m0, m1, s0, s1, mi, mo.T)
    row = jax.ShapeDtypeStruct((1, W), f32)
    wide = jax.ShapeDtypeStruct((8, W), f32)
    short = jax.ShapeDtypeStruct((8, W), bf16)
    outs = pl.pallas_call(
        functools.partial(finish, entries),
        out_shape=(row, row, row, row, wide, wide, wide, wide, short, short),
        in_specs=[vmem] * 4,
        name="finish",
    )(*(pltpu.with_memory_space_constraint(v, pltpu.VMEM) for v in (step, fs, q, old)))
    return tuple(out.T if k in (5, 7, 9) else out for k, out in enumerate(outs))


def solution(mesh):
    ny = mesh.shape["tp"]
    nx = 4
    nz = mesh.shape["fs"] // (2 * nx)
    finer = Mesh(mesh.devices.reshape(nz, nx, 2, ny), (*FS, "tp"))
    rows, cols = P(FS, "tp"), P("tp", FS)
    return jax.shard_map(
        functools.partial(shards, nz, nx, ny),
        mesh=finer,
        in_specs=(P(FS, None), rows, rows, P(FS, None), P(), P(), rows, cols, rows, rows, rows, rows),
        out_specs=(rows, rows, rows, rows, rows, cols, rows, cols, rows, cols),
        check_vma=False,
    )
```
